32 devices in a mesh: grp: 2 (over x), ep: 16 (over z, y, core).
Axes of the slice: x: 2, y: 2, z: 4, core: 2. Of those that a mesh axis runs over, the one named last changes fastest.
Arguments:
- tokens: bfloat16 [1024, 2048], P(('grp', 'ep')), parts along dimension 0, may hold values from -6 to 6
- routing: int32 [1024, 4], P(('grp', 'ep')), parts along dimension 0, may hold values from 0 to 15, as said below
- gate_weights: float32 [1024, 4], P(('grp', 'ep')), parts along dimension 0, may hold values from 0.05 to 1
- pre_gain: float32 [2048], replicated, may hold values from 0.1 to 1.9
- w_gate: bfloat16 [16, 2048, 512], P('ep'), may hold values from -0.125 to 0.125
- w_up: bfloat16 [16, 2048, 512], P('ep'), may hold values from -0.125 to 0.125
- w_down: bfloat16 [16, 512, 2048], P('ep'), may hold values from -0.25 to 0.25
- post_gain: float32 [2048], replicated, may hold values from 0.1 to 1.9
Outputs:
- mixed_out: bfloat16 [1024, 2048], P(('grp', 'ep')), parts along dimension 0
The draws below stay inside these ranges and needn't reach their ends.
There are 2 independent parts, one for each index of `grp`. The reference program is written for one: setup_inputs(seed, part) draws one part's arguments, and reference() takes and returns one part's arrays. A program takes and returns all parts, laid end to end along the dimension named above; an argument that names none is the same for every part. Nothing has to cross between parts.
Inputs may be any that keep to these rules, and one draw needn't show every extreme that they name: `routing`: each row names 4 different experts of one group (experts g * 8 to g * 8 + 7). The rows of one device name any one expert at most 16 times, and some expert exactly 16 times.
All inputs are finite; a program needn't handle non-finite values.
Results may differ from the reference program's by a relative error of at most 0.0085.
Values may be sent and summed in bfloat16 or wider, within the bound.
No kernel may reach another device: no remote copies, remote signals or barrier semaphores. Data moves between devices by JAX's collectives and lax.ppermute only.
A program may use at most 64 MiB of HBM per device.

```python
import math
import jax
import jax.numpy as jnp
from jax import lax

D = 2048
EXPERT_FF = 512
TOPK = 4
EXP_GROUP = 8
TOK_DEV = 32
EXPERTS = 16
SPECIALIST_SETS = 2
CAP = 16
TOKENS = 512
N_EP = 16


def draw_routing(key, part):
    group_slots = 2 * CAP
    slot_count = SPECIALIST_SETS * group_slots
    sampler_seeds = jax.random.split(key, 5)
    affinity_increment = jax.random.permutation(sampler_seeds[0], SPECIALIST_SETS).astype(jnp.int32) * (1024 // SPECIALIST_SETS)
    mandated_cluster = jax.random.randint(sampler_seeds[1], (N_EP,), 0, SPECIALIST_SETS)
    affinity_jitter = jax.random.randint(sampler_seeds[2], (N_EP, slot_count), 0, 1024)
    slot_ids = jnp.arange(slot_count, dtype=jnp.int32)
    cluster_for_position = slot_ids // group_slots
    cluster_affinity = affinity_jitter + affinity_increment[cluster_for_position][None, :] + jnp.where(cluster_for_position[None, :] == mandated_cluster[:, None], 4096, 0)
    cluster_affinity = cluster_affinity * slot_count + slot_ids[None, :]
    chosen = lax.top_k(cluster_affinity, TOK_DEV)[1].astype(jnp.int32)
    shuffle = jax.random.randint(sampler_seeds[3], (N_EP, TOK_DEV), 0, 1 << 20) * TOK_DEV + jnp.arange(TOK_DEV, dtype=jnp.int32)[None, :]
    chosen = jnp.take_along_axis(chosen, jnp.argsort(shuffle, axis=1, stable=True), axis=1)
    group_of = chosen // group_slots
    rank_of = chosen % group_slots
    offsets = jax.random.randint(sampler_seeds[4], (N_EP, SPECIALIST_SETS), 0, EXP_GROUP)
    offset_of = jnp.take_along_axis(offsets, group_of, axis=1)
    within = (offset_of[..., None] + rank_of[..., None] * TOPK + jnp.arange(TOPK, dtype=jnp.int32)) % EXP_GROUP
    return (group_of[..., None] * EXP_GROUP + within).reshape(TOKENS, TOPK).astype(jnp.int32)


def levels(stream_key, shape, cuts, low, largest):
    factor_of, own = 1.0, jax.random.fold_in(stream_key, 6)
    for axis_at, shards_of in cuts:
        heights = jnp.exp(jax.random.uniform(jax.random.fold_in(own, axis_at), (shards_of,), jnp.float32, low / len(cuts), largest / len(cuts)))
        factor_of = factor_of * jnp.repeat(heights, shape[axis_at] // shards_of).reshape([-1 if axis == axis_at else 1 for axis in range(len(shape))])
    return factor_of


def centred(key, extent, spread, bound, shards=(), kind=jnp.bfloat16):
    result = jax.random.normal(key, extent, jnp.float32) * spread
    if len(shards) > 0:
        result = levels(key, extent, shards, -0.22, 0.18) * result
    return jnp.clip(result, min=-bound, max=bound).astype(kind)


def setup_inputs(seed: int = 0, part: int = 0) -> dict:
    streams_of = jax.random.split(jax.random.key(seed), 9)
    part_splits = jax.random.split(jax.random.fold_in(streams_of[8], part), 9)
    return {
        "tokens": centred(part_splits[0], (TOKENS, D), 1.0, 6.0, ((0, 16),)),
        "routing": draw_routing(jax.random.fold_in(jax.random.fold_in(streams_of[8], part), 71), part),
        "gate_weights": jnp.clip(jnp.exp(math.log(1.0) - 2.9957323 * jax.random.uniform(part_splits[2], (TOKENS, TOPK), jnp.float32) ** levels(part_splits[2], (TOKENS, TOPK), ((0, 16),), -0.2, 0.2)), 0.05, 1.0),
        "pre_gain": jnp.clip(1.0 + 0.18 * jax.random.normal(streams_of[3], (D,), jnp.float32), 0.1, 1.9),
        "w_gate": centred(streams_of[4], (EXPERTS, D, EXPERT_FF), D ** -0.5, 0.125, ((0, 16),)),
        "w_up": centred(streams_of[5], (EXPERTS, D, EXPERT_FF), D ** -0.5, 0.125, ((0, 16),)),
        "w_down": centred(streams_of[6], (EXPERTS, EXPERT_FF, D), EXPERT_FF ** -0.5, 0.25, ((0, 16),)),
        "post_gain": jnp.clip(1.0 + 0.18 * jax.random.normal(streams_of[7], (D,), jnp.float32), 0.1, 1.9),
    }


epsilon = 1e-06

def normalize(values, gain):
    floats = values.astype(jnp.float32)
    return floats * lax.rsqrt(lax.optimization_barrier(jnp.mean(floats * floats, axis=-1, keepdims=True)) + epsilon) * gain

def reference(tokens, routing, gate_weights, pre_gain, w_gate, w_up, w_down, post_gain):
    normed = normalize(tokens, pre_gain).astype(jnp.bfloat16)
    flat_expert = routing.reshape(-1).astype(jnp.int32)
    flat_token = jnp.repeat(jnp.arange(TOKENS, dtype=jnp.int32), TOPK)
    flat_weight = gate_weights.reshape(-1)
    order = jnp.argsort(flat_expert, stable=True)
    sorted_token = flat_token[order]
    sorted_weight = flat_weight[order]
    counts = lax.optimization_barrier(jnp.sum((flat_expert[None, :] == jnp.arange(EXPERTS, dtype=jnp.int32)[:, None]).astype(jnp.int32), axis=1))
    starts = (jnp.cumsum(counts) - counts).astype(jnp.int32)
    most = CAP * N_EP
    token_pad = jnp.concatenate([sorted_token, jnp.full((most,), TOKENS, jnp.int32)])
    weight_pad = jnp.concatenate([sorted_weight, jnp.zeros((most,), jnp.float32)])
    normed_pad = jnp.concatenate([normed, jnp.zeros((1, D), normed.dtype)], axis=0)

    def one_expert(carry, expert):
        begin = starts[expert].astype(jnp.int32)
        index_rows = lax.dynamic_slice(token_pad, (begin,), (most,))
        weight_rows = lax.dynamic_slice(weight_pad, (begin,), (most,))
        live = jnp.arange(most) < counts[expert]
        index_rows = jnp.where(live, index_rows, TOKENS).astype(jnp.int32)
        weight_rows = jnp.where(live, weight_rows, 0.0)
        rows = normed_pad[index_rows]
        gate = jnp.dot(rows, w_gate[expert], preferred_element_type=jnp.float32)
        upward = jnp.dot(rows, w_up[expert], preferred_element_type=jnp.float32)
        hidden = (jax.nn.silu(gate) * upward).astype(jnp.bfloat16)
        output = jnp.dot(hidden, w_down[expert], preferred_element_type=jnp.float32).astype(jnp.bfloat16)
        carry = carry.at[index_rows].add(output.astype(jnp.float32) * weight_rows[:, None])
        return (carry, None)
    start_sum = jnp.zeros((TOKENS + 1, D), jnp.float32)
    mixture = lax.scan(one_expert, start_sum, jnp.arange(EXPERTS, dtype=jnp.int32))[0][:TOKENS]
    return normalize(mixture, post_gain).astype(jnp.bfloat16)
```

```python
import jax
import jax.numpy as jnp
from jax import lax
from jax.experimental import pallas as pl
from jax.experimental.pallas import tpu as pltpu
from jax.sharding import PartitionSpec as P

epsilon = 1e-06
QUAD = 4
PARTS = 3


def pack_kernel(tokens_ref, routing_ref, weights_ref, gain_ref, out_ref, *, experts, extra):
    rows, width = tokens_ref.shape
    floats = tokens_ref[...].astype(jnp.float32)
    scale = lax.rsqrt(jnp.mean(floats * floats, axis=-1, keepdims=True) + epsilon)
    out_ref[:, :width] = (floats * scale * gain_ref[...]).astype(jnp.bfloat16)
    expert = lax.broadcasted_iota(jnp.int32, (experts, rows), 0)
    dense = jnp.zeros((experts, rows), jnp.float32)
    for k in range(routing_ref.shape[0]):
        dense = dense + jnp.where(
            routing_ref[k : k + 1, :] == expert, weights_ref[k : k + 1, :], 0.0
        )
    pieces = []
    for _ in range(PARTS):
        piece = dense.astype(jnp.bfloat16)
        pieces.append(piece)
        dense = dense - piece.astype(jnp.float32)
    if extra > PARTS * experts:
        pieces.append(jnp.zeros((extra - PARTS * experts, rows), jnp.bfloat16))
    table = jnp.concatenate(pieces, axis=0)
    eye = (
        lax.broadcasted_iota(jnp.int32, (rows, rows), 0)
        == lax.broadcasted_iota(jnp.int32, (rows, rows), 1)
    ).astype(jnp.bfloat16)
    flipped = lax.dot_general(
        eye, table, (((1,), (1,)), ((), ())), preferred_element_type=jnp.float32
    )
    out_ref[:, width:] = flipped.astype(jnp.bfloat16)


def expert_kernel(
    me_ref, mine_ref, other_ref, gate_ref, up_ref, down_ref, keep_ref, send_ref, *, experts
):
    rows, wide = mine_ref.shape
    width = gate_ref.shape[1]
    both = jnp.concatenate([mine_ref[...], other_ref[...]], axis=0)
    values = both[:, :width]
    table = both[:, width:].astype(jnp.float32)
    lane = lax.broadcasted_iota(jnp.int32, table.shape, 1)
    chosen = (lane % experts == me_ref[0]) & (lane < PARTS * experts)
    weight = jnp.sum(jnp.where(chosen, table, 0.0), axis=1, keepdims=True)
    gate = jnp.dot(values, gate_ref[0], preferred_element_type=jnp.float32)
    upward = jnp.dot(values, up_ref[0], preferred_element_type=jnp.float32)
    hidden = (gate / (1.0 + jnp.exp(-gate)) * upward).astype(jnp.bfloat16)
    served = jnp.dot(hidden, down_ref[0], preferred_element_type=jnp.float32) * weight
    keep_ref[...] = served[:rows]
    send_ref[...] = served[rows:].astype(jnp.bfloat16)


def finish_kernel(*refs):
    *parts, gain_ref, out_ref = refs
    mixture = parts[0][...].astype(jnp.float32)
    for part in parts[1:]:
        mixture = mixture + part[...].astype(jnp.float32)
    scale = lax.rsqrt(jnp.mean(mixture * mixture, axis=-1, keepdims=True) + epsilon)
    out_ref[...] = (mixture * scale * gain_ref[...]).astype(jnp.bfloat16)


def body(tokens, routing, gate_weights, pre_gain, w_gate, w_up, w_down, post_gain):
    rows, width = tokens.shape
    devices = lax.axis_size("ep")
    extra = -(-PARTS * devices // 128) * 128
    slabs = devices // QUAD
    me = lax.axis_index("ep").astype(jnp.int32).reshape(1)

    def swap(values, bits):
        return lax.ppermute(values, "ep", [(i, i ^ bits) for i in range(devices)])

    def kernel(function, outs, **static):
        return pl.pallas_call(
            lambda *refs: function(*refs, **static), out_shape=outs, name=function.__name__
        )

    packed = kernel(
        pack_kernel,
        jax.ShapeDtypeStruct((rows, width + extra), jnp.bfloat16),
        experts=devices,
        extra=extra,
    )(tokens, routing.T, gate_weights.T, pre_gain.reshape(1, width))

    blocks = {j: swap(packed, QUAD * j) for j in reversed(range(1, slabs))}
    blocks[0] = packed
    order = list(reversed(range(1, slabs))) + [0]
    arrived = {}
    for j in [0] + order[:-1]:
        column = jnp.concatenate([blocks[j], swap(blocks[j], 2)], axis=0)
        arrived[j] = (column, swap(column, 1))

    serve = pl.pallas_call(
        lambda *refs: expert_kernel(*refs, experts=devices),
        out_shape=(
            jax.ShapeDtypeStruct((2 * rows, width), jnp.float32),
            jax.ShapeDtypeStruct((2 * rows, width), jnp.bfloat16),
        ),
        in_specs=[pl.BlockSpec(memory_space=pltpu.SMEM)]
        + [pl.BlockSpec(memory_space=pltpu.VMEM)] * 5,
        name="expert_kernel",
    )
    home = {}
    for j in order:
        keep, send = serve(me, *arrived[j], w_gate, w_up, w_down)
        column = keep + swap(send, 1).astype(jnp.float32)
        back = swap(column[rows:].astype(jnp.bfloat16), 2)
        total = column[:rows] + back.astype(jnp.float32)
        home[j] = total if j == 0 else swap(total.astype(jnp.bfloat16), QUAD * j)
    return kernel(finish_kernel, jax.ShapeDtypeStruct((rows, width), jnp.bfloat16))(
        *[home[j] for j in range(slabs)], post_gain.reshape(1, width)
    )


def solution(mesh):
    in_specs = (
        P(("grp", "ep"), None),
        P(("grp", "ep"), None),
        P(("grp", "ep"), None),
        P(),
        P("ep", None, None),
        P("ep", None, None),
        P("ep", None, None),
        P(),
    )
    out_specs = P(("grp", "ep"), None)
    return jax.shard_map(body, mesh=mesh, in_specs=in_specs, out_specs=out_specs, check_vma=False)
```

```python
import jax
import jax.numpy as jnp
from jax import lax
from jax.experimental import pallas as pl
from jax.experimental.pallas import tpu as pltpu
from jax.sharding import PartitionSpec as P

epsilon = 1e-06
QUAD = 4
PARTS = 3


def pack_kernel(
    tokens_hbm, routing_hbm, weights_hbm, gain_hbm, out_ref, tokens_ref, routing_ref, weights_ref,
    gain_ref, sems, *, experts, extra
):
    copies = [
        pltpu.make_async_copy(source, target, sems.at[i])
        for i, (source, target) in enumerate(
            [
                (tokens_hbm, tokens_ref),
                (routing_hbm, routing_ref),
                (weights_hbm, weights_ref),
                (gain_hbm, gain_ref),
            ]
        )
    ]
    for copy in copies:
        copy.start()
    for copy in copies:
        copy.wait()
    rows, width = tokens_ref.shape
    floats = tokens_ref[...].astype(jnp.float32)
    scale = lax.rsqrt(jnp.mean(floats * floats, axis=-1, keepdims=True) + epsilon)
    out_ref[:, :width] = (floats * scale * gain_ref[...]).astype(jnp.bfloat16)
    expert = lax.broadcasted_iota(jnp.int32, (experts, rows), 0)
    dense = jnp.zeros((experts, rows), jnp.float32)
    for k in range(routing_ref.shape[0]):
        dense = dense + jnp.where(
            routing_ref[k : k + 1, :] == expert, weights_ref[k : k + 1, :], 0.0
        )
    pieces = []
    for _ in range(PARTS):
        piece = dense.astype(jnp.bfloat16)
        pieces.append(piece)
        dense = dense - piece.astype(jnp.float32)
    if extra > PARTS * experts:
        pieces.append(jnp.zeros((extra - PARTS * experts, rows), jnp.bfloat16))
    table = jnp.concatenate(pieces, axis=0)
    eye = (
        lax.broadcasted_iota(jnp.int32, (rows, rows), 0)
        == lax.broadcasted_iota(jnp.int32, (rows, rows), 1)
    ).astype(jnp.bfloat16)
    flipped = lax.dot_general(
        eye, table, (((1,), (1,)), ((), ())), preferred_element_type=jnp.float32
    )
    out_ref[:, width:] = flipped.astype(jnp.bfloat16)


def load_kernel(*refs):
    sems = refs[-1]
    count = len(refs) // 2
    copies = [
        pltpu.make_async_copy(refs[i], refs[count + i], sems.at[i]) for i in range(count)
    ]
    for copy in copies:
        copy.start()
    for copy in copies:
        copy.wait()


def expert_kernel(
    me_ref, mine_ref, other_ref, gate_ref, up_ref, down_ref, keep_ref, send_ref, *, experts
):
    rows, _ = mine_ref.shape
    width = gate_ref.shape[1]
    both = jnp.concatenate([mine_ref[...], other_ref[...]], axis=0)
    values = both[:, :width]
    table = both[:, width:].astype(jnp.float32)
    lane = lax.broadcasted_iota(jnp.int32, table.shape, 1)
    chosen = (lane % experts == me_ref[0]) & (lane < PARTS * experts)
    weight = jnp.sum(jnp.where(chosen, table, 0.0), axis=1, keepdims=True)
    gate = jnp.dot(values, gate_ref[0], preferred_element_type=jnp.float32)
    upward = jnp.dot(values, up_ref[0], preferred_element_type=jnp.float32)
    hidden = (gate / (1.0 + jnp.exp(-gate)) * upward).astype(jnp.bfloat16)
    served = jnp.dot(hidden, down_ref[0], preferred_element_type=jnp.float32) * weight
    keep_ref[...] = served[:rows]
    send_ref[...] = served[rows:].astype(jnp.bfloat16)


def finish_kernel(*refs):
    *parts, gain_ref, out_ref = refs
    mixture = parts[0][...].astype(jnp.float32)
    for part in parts[1:]:
        mixture = mixture + part[...].astype(jnp.float32)
    scale = lax.rsqrt(jnp.mean(mixture * mixture, axis=-1, keepdims=True) + epsilon)
    out_ref[...] = (mixture * scale * gain_ref[...]).astype(jnp.bfloat16)


IN_HBM = pl.BlockSpec(memory_space=pltpu.HBM)
IN_VMEM = pl.BlockSpec(memory_space=pltpu.VMEM)
IN_SMEM = pl.BlockSpec(memory_space=pltpu.SMEM)


def low(j):
    return j & -j


def body(tokens, routing, gate_weights, pre_gain, w_gate, w_up, w_down, post_gain):
    rows, width = tokens.shape
    choices = routing.shape[1]
    devices = lax.axis_size("ep")
    extra = -(-PARTS * devices // 128) * 128
    slabs = devices // QUAD
    me = lax.axis_index("ep").astype(jnp.int32).reshape(1)

    def swap(values, bits):
        return lax.ppermute(values, "ep", [(i, i ^ bits) for i in range(devices)])

    packed = pl.pallas_call(
        lambda *refs: pack_kernel(*refs, experts=devices, extra=extra),
        out_shape=jax.ShapeDtypeStruct((rows, width + extra), jnp.bfloat16),
        in_specs=[IN_HBM] * 4,
        out_specs=IN_VMEM,
        scratch_shapes=[
            pltpu.VMEM((rows, width), tokens.dtype),
            pltpu.VMEM((choices, rows), routing.dtype),
            pltpu.VMEM((choices, rows), gate_weights.dtype),
            pltpu.VMEM((1, width), pre_gain.dtype),
            pltpu.SemaphoreType.DMA((4,)),
        ],
        name="pack_kernel",
        compiler_params=pltpu.CompilerParams(vmem_limit_bytes=4 << 20),
    )(tokens, routing.T, gate_weights.T, pre_gain.reshape(1, width))

    blocks = {0: packed}
    for j in range(1, slabs):
        blocks[j] = swap(blocks[j ^ low(j)], QUAD * low(j))

    weights = pl.pallas_call(
        load_kernel,
        out_shape=[jax.ShapeDtypeStruct(w.shape, w.dtype) for w in (w_gate, w_up, w_down)],
        in_specs=[IN_HBM] * 3,
        out_specs=[IN_VMEM] * 3,
        scratch_shapes=[pltpu.SemaphoreType.DMA((3,))],
        name="load_kernel",
        compiler_params=pltpu.CompilerParams(vmem_limit_bytes=16 << 20),
    )(w_gate, w_up, w_down)

    serve = pl.pallas_call(
        lambda *refs: expert_kernel(*refs, experts=devices),
        out_shape=(
            jax.ShapeDtypeStruct((2 * rows, width), jnp.float32),
            jax.ShapeDtypeStruct((2 * rows, width), jnp.bfloat16),
        ),
        in_specs=[IN_SMEM] + [IN_VMEM] * 5,
        name="expert_kernel",
        compiler_params=pltpu.CompilerParams(vmem_limit_bytes=16 << 20),
    )
    home = {}
    for j in range(slabs):
        column = jnp.concatenate([blocks[j], swap(blocks[j], 2)], axis=0)
        other = swap(column, 1)
        keep, send = serve(me, column, other, *weights)
        column = keep + swap(send, 1).astype(jnp.float32)
        back = swap(column[rows:].astype(jnp.bfloat16), 2)
        total = column[:rows] + back.astype(jnp.float32)
        home[j] = total if j == 0 else swap(total.astype(jnp.bfloat16), QUAD * j)
    return pl.pallas_call(
        finish_kernel,
        out_shape=jax.ShapeDtypeStruct((rows, width), jnp.bfloat16),
        name="finish_kernel",
        compiler_params=pltpu.CompilerParams(vmem_limit_bytes=4 << 20),
    )(*[home[j] for j in range(slabs)], post_gain.reshape(1, width))


def solution(mesh):
    in_specs = (
        P(("grp", "ep"), None),
        P(("grp", "ep"), None),
        P(("grp", "ep"), None),
        P(),
        P("ep", None, None),
        P("ep", None, None),
        P("ep", None, None),
        P(),
    )
    out_specs = P(("grp", "ep"), None)

    return jax.shard_map(body, mesh=mesh, in_specs=in_specs, out_specs=out_specs, check_vma=False)
```

```python
import jax
import jax.numpy as jnp
from jax import lax
from jax.experimental import pallas as pl
from jax.experimental.pallas import tpu as pltpu
from jax.sharding import PartitionSpec as P

epsilon = 1e-06
QUAD = 4
PARTS = 3


def pack_kernel(
    tokens_hbm, routing_hbm, weights_hbm, gain_hbm, out_ref, tokens_ref, routing_ref, weights_ref,
    gain_ref, sems, *, experts, extra
):
    copies = [
        pltpu.make_async_copy(source, target, sems.at[i])
        for i, (source, target) in enumerate(
            [
                (tokens_hbm, tokens_ref),
                (routing_hbm, routing_ref),
                (weights_hbm, weights_ref),
                (gain_hbm, gain_ref),
            ]
        )
    ]
    for copy in copies:
        copy.start()
    for copy in copies:
        copy.wait()
    rows, width = tokens_ref.shape
    floats = tokens_ref[...].astype(jnp.float32)
    scale = lax.rsqrt(jnp.mean(floats * floats, axis=-1, keepdims=True) + epsilon)
    out_ref[:, :width] = (floats * scale * gain_ref[...]).astype(jnp.bfloat16)
    expert = lax.broadcasted_iota(jnp.int32, (experts, rows), 0)
    dense = jnp.zeros((experts, rows), jnp.float32)
    for k in range(routing_ref.shape[0]):
        dense = dense + jnp.where(
            routing_ref[k : k + 1, :] == expert, weights_ref[k : k + 1, :], 0.0
        )
    pieces = []
    for _ in range(PARTS):
        piece = dense.astype(jnp.bfloat16)
        pieces.append(piece)
        dense = dense - piece.astype(jnp.float32)
    if extra > PARTS * experts:
        pieces.append(jnp.zeros((extra - PARTS * experts, rows), jnp.bfloat16))
    table = jnp.concatenate(pieces, axis=0)
    eye = (
        lax.broadcasted_iota(jnp.int32, (rows, rows), 0)
        == lax.broadcasted_iota(jnp.int32, (rows, rows), 1)
    ).astype(jnp.bfloat16)
    flipped = lax.dot_general(
        eye, table, (((1,), (1,)), ((), ())), preferred_element_type=jnp.float32
    )
    out_ref[:, width:] = flipped.astype(jnp.bfloat16)


def load_kernel(*refs):
    sems = refs[-1]
    count = len(refs) // 2
    copies = [
        pltpu.make_async_copy(refs[i], refs[count + i], sems.at[i]) for i in range(count)
    ]
    for copy in copies:
        copy.start()
    for copy in copies:
        copy.wait()


def expert_kernel(
    me_ref, mine_ref, other_ref, gate_ref, up_ref, down_ref, keep_ref, send_ref, *, experts
):
    rows, _ = mine_ref.shape
    width = gate_ref.shape[1]
    both = jnp.concatenate([mine_ref[...], other_ref[...]], axis=0)
    values = both[:, :width]
    table = both[:, width:].astype(jnp.float32)
    lane = lax.broadcasted_iota(jnp.int32, table.shape, 1)
    chosen = (lane % experts == me_ref[0]) & (lane < PARTS * experts)
    weight = jnp.sum(jnp.where(chosen, table, 0.0), axis=1, keepdims=True)
    gate = jnp.dot(values, gate_ref[0], preferred_element_type=jnp.float32)
    upward = jnp.dot(values, up_ref[0], preferred_element_type=jnp.float32)
    hidden = (gate / (1.0 + jnp.exp(-gate)) * upward).astype(jnp.bfloat16)
    served = jnp.dot(hidden, down_ref[0], preferred_element_type=jnp.float32) * weight
    keep_ref[...] = served[:rows]
    send_ref[...] = served[rows:].astype(jnp.bfloat16)


def finish_kernel(*refs):
    *parts, gain_ref, out_ref = refs
    mixture = parts[0][...].astype(jnp.float32)
    for part in parts[1:]:
        mixture = mixture + part[...].astype(jnp.float32)
    scale = lax.rsqrt(jnp.mean(mixture * mixture, axis=-1, keepdims=True) + epsilon)
    out_ref[...] = (mixture * scale * gain_ref[...]).astype(jnp.bfloat16)


def in_hbm(values):
    return pltpu.with_memory_space_constraint(values, pltpu.HBM)


IN_HBM = pl.BlockSpec(memory_space=pltpu.HBM)
IN_VMEM = pl.BlockSpec(memory_space=pltpu.VMEM)
IN_SMEM = pl.BlockSpec(memory_space=pltpu.SMEM)


def low(j):
    return j & -j


def body(tokens, routing, gate_weights, pre_gain, w_gate, w_up, w_down, post_gain):
    rows, width = tokens.shape
    choices = routing.shape[1]
    devices = lax.axis_size("ep")
    extra = -(-PARTS * devices // 128) * 128
    slabs = devices // QUAD
    me = lax.axis_index("ep").astype(jnp.int32).reshape(1)

    def swap(values, bits):
        return lax.ppermute(values, "ep", [(i, i ^ bits) for i in range(devices)])

    packed = pl.pallas_call(
        lambda *refs: pack_kernel(*refs, experts=devices, extra=extra),
        out_shape=jax.ShapeDtypeStruct((rows, width + extra), jnp.bfloat16),
        in_specs=[IN_HBM] * 4,
        out_specs=IN_VMEM,
        scratch_shapes=[
            pltpu.VMEM((rows, width), tokens.dtype),
            pltpu.VMEM((choices, rows), routing.dtype),
            pltpu.VMEM((choices, rows), gate_weights.dtype),
            pltpu.VMEM((1, width), pre_gain.dtype),
            pltpu.SemaphoreType.DMA((4,)),
        ],
        name="pack_kernel",
        compiler_params=pltpu.CompilerParams(vmem_limit_bytes=4 << 20),
    )(*map(in_hbm, (tokens, routing.T, gate_weights.T, pre_gain.reshape(1, width))))

    blocks = {0: packed}
    for j in range(1, slabs):
        blocks[j] = swap(blocks[j ^ low(j)], QUAD * low(j))

    weights = pl.pallas_call(
        load_kernel,
        out_shape=[jax.ShapeDtypeStruct(w.shape, w.dtype) for w in (w_gate, w_up, w_down)],
        in_specs=[IN_HBM] * 3,
        out_specs=[IN_VMEM] * 3,
        scratch_shapes=[pltpu.SemaphoreType.DMA((3,))],
        name="load_kernel",
        compiler_params=pltpu.CompilerParams(vmem_limit_bytes=4 << 20),
    )(*map(in_hbm, (w_gate, w_up, w_down)))

    serve = pl.pallas_call(
        lambda *refs: expert_kernel(*refs, experts=devices),
        out_shape=(
            jax.ShapeDtypeStruct((2 * rows, width), jnp.float32),
            jax.ShapeDtypeStruct((2 * rows, width), jnp.bfloat16),
        ),
        in_specs=[IN_SMEM] + [IN_VMEM] * 5,
        name="expert_kernel",
        compiler_params=pltpu.CompilerParams(vmem_limit_bytes=16 << 20),
    )
    home = {}
    for j in range(slabs):
        column = jnp.concatenate([blocks[j], swap(blocks[j], 2)], axis=0)
        other = swap(column, 1)
        keep, send = serve(me, column, other, *weights)
        column = keep + swap(send, 1).astype(jnp.float32)
        back = swap(column[rows:].astype(jnp.bfloat16), 2)
        total = column[:rows] + back.astype(jnp.float32)
        home[j] = total if j == 0 else swap(total.astype(jnp.bfloat16), QUAD * j)
    return pl.pallas_call(
        finish_kernel,
        out_shape=jax.ShapeDtypeStruct((rows, width), jnp.bfloat16),
        name="finish_kernel",
        compiler_params=pltpu.CompilerParams(vmem_limit_bytes=4 << 20),
    )(*[home[j] for j in range(slabs)], post_gain.reshape(1, width))


def solution(mesh):
    in_specs = (
        P(("grp", "ep"), None),
        P(("grp", "ep"), None),
        P(("grp", "ep"), None),
        P(),
        P("ep", None, None),
        P("ep", None, None),
        P("ep", None, None),
        P(),
    )
    out_specs = P(("grp", "ep"), None)

    return jax.shard_map(body, mesh=mesh, in_specs=in_specs, out_specs=out_specs, check_vma=False)
```

```python
import jax
import jax.numpy as jnp
from jax import lax
from jax.experimental import pallas as pl
from jax.experimental.pallas import tpu as pltpu
from jax.sharding import PartitionSpec as P

epsilon = 1e-06
QUAD = 4
PARTS = 3
MERGE = 2


def pack_kernel(
    me_ref, tokens_hbm, routing_hbm, weights_hbm, gain_hbm, out_ref, place_ref, tokens_ref, routing_ref, weights_ref,
    gain_ref, sems, *, experts, extra
):
    copies = [
        pltpu.make_async_copy(source, target, sems.at[i])
        for i, (source, target) in enumerate(
            [
                (tokens_hbm, tokens_ref),
                (routing_hbm, routing_ref),
                (weights_hbm, weights_ref),
                (gain_hbm, gain_ref),
            ]
        )
    ]
    for copy in copies:
        copy.start()
    for copy in copies:
        copy.wait()
    place_ref[...] = jnp.full(place_ref.shape, me_ref[0], jnp.int32)
    rows, width = tokens_ref.shape
    floats = tokens_ref[...].astype(jnp.float32)
    scale = lax.rsqrt(jnp.mean(floats * floats, axis=-1, keepdims=True) + epsilon)
    out_ref[:, :width] = (floats * scale * gain_ref[...]).astype(jnp.bfloat16)
    expert = lax.broadcasted_iota(jnp.int32, (experts, rows), 0)
    dense = jnp.zeros((experts, rows), jnp.float32)
    for k in range(routing_ref.shape[0]):
        dense = dense + jnp.where(
            routing_ref[k : k + 1, :] == expert, weights_ref[k : k + 1, :], 0.0
        )
    pieces = []
    for _ in range(PARTS):
        piece = dense.astype(jnp.bfloat16)
        pieces.append(piece)
        dense = dense - piece.astype(jnp.float32)
    if extra > PARTS * experts:
        pieces.append(jnp.zeros((extra - PARTS * experts, rows), jnp.bfloat16))
    table = jnp.concatenate(pieces, axis=0)
    eye = (
        lax.broadcasted_iota(jnp.int32, (rows, rows), 0)
        == lax.broadcasted_iota(jnp.int32, (rows, rows), 1)
    ).astype(jnp.bfloat16)
    flipped = lax.dot_general(
        eye, table, (((1,), (1,)), ((), ())), preferred_element_type=jnp.float32
    )
    out_ref[:, width:] = flipped.astype(jnp.bfloat16)


def load_kernel(*refs):
    sems = refs[-1]
    count = len(refs) // 2
    copies = [
        pltpu.make_async_copy(refs[i], refs[count + i], sems.at[i]) for i in range(count)
    ]
    for copy in copies:
        copy.start()
    for copy in copies:
        copy.wait()


def expert_kernel(*refs, experts, count):
    place_ref, blocks, rest = refs[0], refs[1 : 1 + 2 * count], refs[1 + 2 * count :]
    weights, outs = rest[:6], rest[6:]
    rows, width = outs[0].shape
    both = jnp.concatenate([block[...] for block in blocks], axis=0)
    values = both[:, :width]
    table = both[:, width:].astype(jnp.float32)
    lane = lax.broadcasted_iota(jnp.int32, table.shape, 1)
    total = None
    for bit, (gate_ref, up_ref, down_ref) in enumerate((weights[:3], weights[3:])):
        chosen = (lane % experts == (place_ref[:, :1] ^ bit)) & (lane < PARTS * experts)
        weight = jnp.sum(jnp.where(chosen, table, 0.0), axis=1, keepdims=True)
        gate = jnp.dot(values, gate_ref[0], preferred_element_type=jnp.float32)
        upward = jnp.dot(values, up_ref[0], preferred_element_type=jnp.float32)
        hidden = (gate / (1.0 + jnp.exp(-gate)) * upward).astype(jnp.bfloat16)
        served = jnp.dot(hidden, down_ref[0], preferred_element_type=jnp.float32) * weight
        total = served if total is None else total + served
    for i in range(count):
        outs[i][...] = total[i * rows : (i + 1) * rows]
        outs[count + i][...] = total[(count + i) * rows : (count + i + 1) * rows].astype(
            jnp.bfloat16
        )


def finish_kernel(*refs):
    *parts, gain_ref, out_ref = refs
    mixture = parts[0][...].astype(jnp.float32)
    for part in parts[1:]:
        mixture = mixture + part[...].astype(jnp.float32)
    scale = lax.rsqrt(jnp.mean(mixture * mixture, axis=-1, keepdims=True) + epsilon)
    out_ref[...] = (mixture * scale * gain_ref[...]).astype(jnp.bfloat16)


def in_hbm(values):
    return pltpu.with_memory_space_constraint(values, pltpu.HBM)


IN_HBM = pl.BlockSpec(memory_space=pltpu.HBM)
IN_VMEM = pl.BlockSpec(memory_space=pltpu.VMEM)
IN_SMEM = pl.BlockSpec(memory_space=pltpu.SMEM)


def low(j):
    return j & -j


def groups_of(slabs):
    first = min(MERGE, slabs)
    return {0: tuple(range(first))} | {j: (j,) for j in range(first, slabs)}


def body(tokens, routing, gate_weights, pre_gain, w_gate, w_up, w_down, post_gain):
    rows, width = tokens.shape
    devices = lax.axis_size("ep")
    choices = routing.shape[1]
    extra = -(-PARTS * devices // 128) * 128
    slabs = devices // QUAD
    me = lax.axis_index("ep").astype(jnp.int32).reshape(1)

    def swap(values, bits):
        return lax.ppermute(values, "ep", [(i, i ^ bits) for i in range(devices)])

    packed, place = pl.pallas_call(
        lambda *refs: pack_kernel(*refs, experts=devices, extra=extra),
        out_shape=(
            jax.ShapeDtypeStruct((rows, width + extra), jnp.bfloat16),
            jax.ShapeDtypeStruct((1, 128), jnp.int32),
        ),
        in_specs=[IN_SMEM] + [IN_HBM] * 4,
        out_specs=(IN_VMEM, IN_VMEM),
        scratch_shapes=[
            pltpu.VMEM((rows, width), tokens.dtype),
            pltpu.VMEM((choices, rows), routing.dtype),
            pltpu.VMEM((choices, rows), gate_weights.dtype),
            pltpu.VMEM((1, width), pre_gain.dtype),
            pltpu.SemaphoreType.DMA((4,)),
        ],
        name="pack_kernel",
        compiler_params=pltpu.CompilerParams(vmem_limit_bytes=4 << 20),
    )(me, *map(in_hbm, (tokens, routing.T, gate_weights.T, pre_gain.reshape(1, width))))

    blocks = {0: packed}
    for j in range(1, slabs):
        blocks[j] = swap(blocks[j ^ low(j)], QUAD * low(j))

    weights = pl.pallas_call(
        load_kernel,
        out_shape=[jax.ShapeDtypeStruct(w.shape, w.dtype) for w in (w_gate, w_up, w_down)],
        in_specs=[IN_HBM] * 3,
        out_specs=[IN_VMEM] * 3,
        scratch_shapes=[pltpu.SemaphoreType.DMA((3,))],
        name="load_kernel",
        compiler_params=pltpu.CompilerParams(vmem_limit_bytes=4 << 20),
    )(*map(in_hbm, (w_gate, w_up, w_down)))

    weights = [*weights] + [swap(w, 1) for w in (w_gate, w_up, w_down)]

    across = {j: swap(blocks[j], 2) for j in range(slabs)}
    home = {}
    for members in groups_of(slabs).values():
        count = len(members)
        served = pl.pallas_call(
            lambda *refs: expert_kernel(*refs, experts=devices, count=count),
            out_shape=[jax.ShapeDtypeStruct((rows, width), jnp.float32)] * count
            + [jax.ShapeDtypeStruct((rows, width), jnp.bfloat16)] * count,
            in_specs=[IN_VMEM] * (7 + 2 * count),
            name="expert_kernel",
            compiler_params=pltpu.CompilerParams(vmem_limit_bytes=20 << 20),
        )(place, *[blocks[j] for j in members], *[across[j] for j in members], *weights)
        for j, keep, send in zip(members, served[:count], served[count:]):
            total = keep + swap(send, 2).astype(jnp.float32)
            home[j] = swap(total.astype(jnp.bfloat16), QUAD * j) if j else total
    return pl.pallas_call(
        finish_kernel,
        out_shape=jax.ShapeDtypeStruct((rows, width), jnp.bfloat16),
        name="finish_kernel",
        compiler_params=pltpu.CompilerParams(vmem_limit_bytes=4 << 20),
    )(*[home[j] for j in range(slabs)], post_gain.reshape(1, width))


def solution(mesh):
    in_specs = (
        P(("grp", "ep"), None),
        P(("grp", "ep"), None),
        P(("grp", "ep"), None),
        P(),
        P("ep", None, None),
        P("ep", None, None),
        P("ep", None, None),
        P(),
    )
    out_specs = P(("grp", "ep"), None)

    return jax.shard_map(body, mesh=mesh, in_specs=in_specs, out_specs=out_specs, check_vma=False)
```

```python
import jax
import jax.numpy as jnp
from jax import lax
from jax.experimental import pallas as pl
from jax.experimental.pallas import tpu as pltpu
from jax.sharding import PartitionSpec as P

epsilon = 1e-06
QUAD = 4
PARTS = 3
MERGE = 2
FILL = 128


def pack_kernel(
    tokens_hbm, routing_hbm, weights_hbm, gain_hbm, out_ref, place_ref, tokens_ref, routing_ref, weights_ref,
    gain_ref, sems, *, experts, extra
):
    copies = [
        pltpu.make_async_copy(source, target, sems.at[i])
        for i, (source, target) in enumerate(
            [
                (tokens_hbm, tokens_ref),
                (routing_hbm, routing_ref),
                (weights_hbm, weights_ref),
                (gain_hbm, gain_ref),
            ]
        )
    ]
    for copy in copies:
        copy.start()
    for copy in copies:
        copy.wait()
    place_ref[...] = jnp.full(place_ref.shape, lax.axis_index("ep"), jnp.int32)
    rows, width = tokens_ref.shape
    floats = tokens_ref[...].astype(jnp.float32)
    scale = lax.rsqrt(jnp.mean(floats * floats, axis=-1, keepdims=True) + epsilon)
    out_ref[:, :width] = (floats * scale * gain_ref[...]).astype(jnp.bfloat16)
    expert = lax.broadcasted_iota(jnp.int32, (experts, rows), 0)
    dense = jnp.zeros((experts, rows), jnp.float32)
    for k in range(routing_ref.shape[0]):
        dense = dense + jnp.where(
            routing_ref[k : k + 1, :] == expert, weights_ref[k : k + 1, :], 0.0
        )
    pieces = []
    for _ in range(PARTS):
        piece = dense.astype(jnp.bfloat16)
        pieces.append(piece)
        dense = dense - piece.astype(jnp.float32)
    if extra > PARTS * experts:
        pieces.append(jnp.zeros((extra - PARTS * experts, rows), jnp.bfloat16))
    table = jnp.concatenate(pieces, axis=0)
    eye = (
        lax.broadcasted_iota(jnp.int32, (rows, rows), 0)
        == lax.broadcasted_iota(jnp.int32, (rows, rows), 1)
    ).astype(jnp.bfloat16)
    flipped = lax.dot_general(
        eye, table, (((1,), (1,)), ((), ())), preferred_element_type=jnp.float32
    )
    out_ref[:, width:] = flipped.astype(jnp.bfloat16)


def load_kernel(*refs):
    sems = refs[-1]
    count = len(refs) // 2
    copies = [
        pltpu.make_async_copy(refs[i], refs[count + i], sems.at[i]) for i in range(count)
    ]
    for copy in copies:
        copy.start()
    for copy in copies:
        copy.wait()


def expert_kernel(place_ref, *refs, experts, count):
    blocks, weights, outs = refs[: 2 * count], refs[2 * count :][:6], refs[2 * count + 6 :]
    rows, width = outs[0].shape
    both = jnp.concatenate([block[...] for block in blocks], axis=0)
    if both.shape[0] < FILL:
        both = jnp.concatenate([both] * (FILL // both.shape[0]), axis=0)
    values = both[:, :width]
    table = both[:, width:].astype(jnp.float32)
    lane = lax.broadcasted_iota(jnp.int32, table.shape, 1)
    hiddens, shares = [], []
    for bit in range(2):
        gate_ref, up_ref, _ = weights[3 * bit : 3 * bit + 3]
        chosen = (lane % experts == (place_ref[:, :1] ^ bit)) & (lane < PARTS * experts)
        shares.append(jnp.sum(jnp.where(chosen, table, 0.0), axis=1, keepdims=True))
        gate = jnp.dot(values, gate_ref[0], preferred_element_type=jnp.float32)
        upward = jnp.dot(values, up_ref[0], preferred_element_type=jnp.float32)
        hiddens.append((gate / (1.0 + jnp.exp(-gate)) * upward).astype(jnp.bfloat16))
    first, second = [
        jnp.dot(hidden, weights[3 * bit + 2][0], preferred_element_type=jnp.float32)
        for bit, hidden in enumerate(hiddens)
    ]
    total = first * shares[0] + second * shares[1]
    for i in range(count):
        own = total[i * rows : (i + 1) * rows]
        other = total[(count + i) * rows : (count + i + 1) * rows]
        if i == 0:
            outs[0][...] = own
            outs[1][...] = other.astype(outs[1].dtype)
        else:
            outs[1 + i][:rows] = own.astype(outs[1 + i].dtype)
            outs[1 + i][rows:] = other.astype(outs[1 + i].dtype)


def finish_kernel(*refs):
    *parts, gain_ref, out_ref = refs
    rows = out_ref.shape[0]
    mixture = parts[0][...].astype(jnp.float32)
    for part in parts[1:]:
        mixture = mixture + part[:rows].astype(jnp.float32)
    scale = lax.rsqrt(jnp.mean(mixture * mixture, axis=-1, keepdims=True) + epsilon)
    out_ref[...] = (mixture * scale * gain_ref[...]).astype(jnp.bfloat16)


def in_hbm(values):
    return pltpu.with_memory_space_constraint(values, pltpu.HBM)


IN_HBM = pl.BlockSpec(memory_space=pltpu.HBM)
IN_VMEM = pl.BlockSpec(memory_space=pltpu.VMEM)


def low(j):
    return j & -j


def groups_of(slabs):
    first = min(MERGE, slabs)
    return {0: tuple(range(first))} | {j: (j,) for j in range(first, slabs)}


def body(tokens, routing, gate_weights, pre_gain, w_gate, w_up, w_down, post_gain):
    rows, width = tokens.shape
    devices = lax.axis_size("ep")
    choices = routing.shape[1]
    extra = -(-PARTS * devices // 128) * 128
    slabs = devices // QUAD

    def swap(values, bits):
        return lax.ppermute(values, "ep", [(i, i ^ bits) for i in range(devices)])

    packed, place = pl.pallas_call(
        lambda *refs: pack_kernel(*refs, experts=devices, extra=extra),
        out_shape=(
            jax.ShapeDtypeStruct((rows, width + extra), jnp.bfloat16),
            jax.ShapeDtypeStruct((1, 128), jnp.int32),
        ),
        in_specs=[IN_HBM] * 4,
        out_specs=(IN_VMEM, IN_VMEM),
        scratch_shapes=[
            pltpu.VMEM((rows, width), tokens.dtype),
            pltpu.VMEM((choices, rows), routing.dtype),
            pltpu.VMEM((choices, rows), gate_weights.dtype),
            pltpu.VMEM((1, width), pre_gain.dtype),
            pltpu.SemaphoreType.DMA((4,)),
        ],
        name="pack_kernel",
        compiler_params=pltpu.CompilerParams(vmem_limit_bytes=4 << 20),
    )(*map(in_hbm, (tokens, routing.T, gate_weights.T, pre_gain.reshape(1, width))))

    blocks, across = {0: packed}, {0: swap(packed, 2)}
    for j in range(1, slabs):
        bits, parent = QUAD * low(j), j ^ low(j)
        blocks[j] = swap(blocks[parent], bits)
        if parent:
            across[j] = swap(across[parent], bits)
        else:
            across[j] = swap(blocks[j], 2)

    weights = pl.pallas_call(
        load_kernel,
        out_shape=[jax.ShapeDtypeStruct(w.shape, w.dtype) for w in (w_gate, w_up, w_down)],
        in_specs=[IN_HBM] * 3,
        out_specs=[IN_VMEM] * 3,
        scratch_shapes=[pltpu.SemaphoreType.DMA((3,))],
        name="load_kernel",
        compiler_params=pltpu.CompilerParams(vmem_limit_bytes=4 << 20),
    )(*map(in_hbm, (w_gate, w_up, w_down)))

    weights = [*weights] + [swap(w, 1) for w in (w_gate, w_up, w_down)]

    home = []
    for g, members in groups_of(slabs).items():
        count = len(members)
        own, other, *near = pl.pallas_call(
            lambda *refs: expert_kernel(*refs, experts=devices, count=count),
            out_shape=[
                jax.ShapeDtypeStruct((rows, width), jnp.float32),
                jax.ShapeDtypeStruct((rows, width), jnp.float32 if g == 0 else jnp.bfloat16),
            ]
            + [jax.ShapeDtypeStruct((2 * rows, width), jnp.bfloat16)] * (count - 1),
            in_specs=[IN_VMEM] * (7 + 2 * count),
            name="expert_kernel",
            compiler_params=pltpu.CompilerParams(vmem_limit_bytes=20 << 20),
        )(place, *[blocks[j] for j in members], *[across[j] for j in members], *weights)
        near = [swap(part, QUAD * j) for j, part in zip(members[1:], near)]
        for part in near:
            other = other + part[rows:].astype(jnp.float32)
        back = swap(other.astype(jnp.bfloat16), 2)
        if g:
            total = (own + back.astype(jnp.float32)).astype(jnp.bfloat16)
            home.append(swap(total, QUAD * g))
        else:
            home += [own, back, *near]
    return pl.pallas_call(
        finish_kernel,
        out_shape=jax.ShapeDtypeStruct((rows, width), jnp.bfloat16),
        name="finish_kernel",
        compiler_params=pltpu.CompilerParams(vmem_limit_bytes=4 << 20),
    )(*home, post_gain.reshape(1, width))


def solution(mesh):
    in_specs = (
        P(("grp", "ep"), None),
        P(("grp", "ep"), None),
        P(("grp", "ep"), None),
        P(),
        P("ep", None, None),
        P("ep", None, None),
        P("ep", None, None),
        P(),
    )
    out_specs = P(("grp", "ep"), None)

    return jax.shard_map(body, mesh=mesh, in_specs=in_specs, out_specs=out_specs, check_vma=False)
```
